32 devices in a mesh: sp: 16 (over z, y, x), tp: 2 (over core).
Axes of the slice: x: 2, y: 2, z: 4, core: 2. Of those that a mesh axis runs over, the one named last changes fastest.
Arguments:
- layer_source_tokens: bfloat16 [2, 1024, 4096], P(None, 'sp'), may hold values from -6 to 6
- address_projection: bfloat16 [4096, 2048], P('sp', 'tp'), may hold values from -0.09375 to 0.09375
- content_projection: bfloat16 [4096, 2048], P('sp', 'tp'), may hold values from -0.09375 to 0.09375
- strength_projection: bfloat16 [4096, 16], replicated, may hold values from -0.09375 to 0.09375
- fading_driver_projection: bfloat16 [4096, 16], replicated, may hold values from -0.25 to 0.25
- strength_offset: float32 [16], P('tp'), may hold values from -2.5 to 1
- channel_fading_speed: float32 [16], P('tp')
- added_fading_exponent: float32 [2, 1024, 16], P(None, 'sp', 'tp'), may hold values from -0.7 to 0, as said below
- first_step_probe: bfloat16 [2, 2048], P(None, 'tp'), may hold values from -6 to 6
- first_step_address: bfloat16 [2, 2048], P(None, 'tp'), may hold values from -6 to 6
- first_step_content: bfloat16 [2, 2048], P(None, 'tp'), may hold values from -6 to 6
- first_step_outgate: bfloat16 [2, 2048], P(None, 'tp'), may hold values from -6 to 6
- first_step_strength_raw: float32 [2, 16], P(None, 'tp'), may hold values from -6 to 6
- channel_scaling_factor: float32 [128], replicated, may hold values from 0.1 to 1.9
- readout_projection: bfloat16 [2048, 4096], P('tp', 'sp'), may hold values from -0.125 to 0.125
Outputs:
- state_cache: bfloat16 [2, 16, 128, 128], P(None, 'tp')
- mixed_read: bfloat16 [2, 4096], P(None, 'sp')
- boundary_cache: bfloat16 [2, 16, 16, 128, 128], P(None, 'sp', 'tp')
The draws below stay inside these ranges and needn't reach their ends.
Inputs may be any that keep to these rules, and one draw needn't show every extreme that they name: `added_fading_exponent`: zero at most positions.
All inputs are finite; a program needn't handle non-finite values.
Results may differ from the reference program's by a relative error of at most 0.017.
Values may be sent and summed in bfloat16 or wider, within the bound.
A program may use at most 64 MiB of HBM per device.

```python
import jax
import jax.numpy as jnp
from jax import lax

D = 4096
H = 16
ADDRESS_WIDTH = 128
BLOCK = 64
NSEQ = 2
LEN = 1024
RANGES = 16
N_TP = 2


def draw_channel_fading_speed(key, part):
    low_rate = 0.3 / LEN
    high_rate = 0.05
    uniform_draw = jax.random.uniform(jax.random.fold_in(key, 11), (H,), jnp.float32)
    return jnp.exp(jnp.log(low_rate) + uniform_draw * (jnp.log(high_rate) - jnp.log(low_rate)))


def draw_added_fading_exponent(key, part):
    chosen = jax.random.uniform(jax.random.fold_in(key, 21), (NSEQ, LEN, H), jnp.float32)
    kept_share = jax.random.uniform(jax.random.fold_in(key, 22), (NSEQ, LEN, H), jnp.float32, 0.5, 0.8)
    return jnp.where(chosen < 3.0 / LEN, jnp.log(kept_share), 0.0)


def block_levels(rng, shape, shards, low, top_value):
    factor_of = 1.0
    for position, shards_of in shards:
        steps = jax.random.uniform(jax.random.fold_in(jax.random.fold_in(rng, 6), position), (shards_of,), jnp.float32, low / len(shards), top_value / len(shards))
        factor_of = factor_of * jnp.repeat(jnp.exp(steps), shape[position] // shards_of).reshape((-1,) + (1,) * (len(shape) - 1 - position))
    return factor_of


def centred(own_key, dims, width, most, shards=(), kind=jnp.bfloat16):
    drawn = width * jax.random.normal(own_key, dims, jnp.float32)
    if shards:
        drawn = drawn * block_levels(own_key, dims, shards, -0.22, 0.18)
    return jnp.clip(drawn, -most, most).astype(kind)


def setup_inputs(seed: int = 0) -> dict:
    key_list = jax.random.split(jax.random.key(seed), 16)
    layer_source_tokens = centred(key_list[0], (NSEQ, LEN, D), 1.0, 6.0, ((1, 16),))
    address_projection = centred(key_list[1], (D, H * ADDRESS_WIDTH), D ** -0.5, 0.09375, ((0, 16), (1, 2)))
    content_projection = centred(key_list[2], (D, H * ADDRESS_WIDTH), D ** -0.5, 0.09375, ((0, 16), (1, 2)))
    strength_projection = centred(key_list[3], (D, H), D ** -0.5, 0.09375)
    fading_driver_projection = centred(key_list[4], (D, H), (D // 9) ** -0.5, 0.25)
    strength_offset = jnp.clip(-2.5 + 3.5 * jax.random.uniform(key_list[5], (H,), jnp.float32) ** block_levels(key_list[5], (H,), ((0, 2),), -0.2, 0.2), -2.5, 1.0)
    channel_fading_speed = draw_channel_fading_speed(jax.random.fold_in(key_list[15], 71), 0)
    added_fading_exponent = draw_added_fading_exponent(jax.random.fold_in(key_list[15], 71), 0)
    first_step_probe = centred(key_list[8], (NSEQ, H * ADDRESS_WIDTH), 1.0, 6.0, ((1, 2),))
    first_step_address = centred(key_list[9], (NSEQ, H * ADDRESS_WIDTH), 1.0, 6.0, ((1, 2),))
    first_step_content = centred(key_list[10], (NSEQ, H * ADDRESS_WIDTH), 1.0, 6.0, ((1, 2),))
    first_step_outgate = centred(key_list[11], (NSEQ, H * ADDRESS_WIDTH), 1.0, 6.0, ((1, 2),))
    first_step_strength_raw = centred(key_list[12], (NSEQ, H), 1.5, 6.0, ((1, 2),), jnp.float32)
    channel_scaling_factor = jnp.clip(1.0 + 0.18 * jax.random.normal(key_list[13], (ADDRESS_WIDTH,), jnp.float32), 0.1, 1.9)
    readout_projection = centred(key_list[14], (H * ADDRESS_WIDTH, D), (H * ADDRESS_WIDTH) ** -0.5, 0.125, ((0, 2), (1, 16)))
    return {"layer_source_tokens": layer_source_tokens, "address_projection": address_projection, "content_projection": content_projection, "strength_projection": strength_projection, "fading_driver_projection": fading_driver_projection, "strength_offset": strength_offset, "channel_fading_speed": channel_fading_speed, "added_fading_exponent": added_fading_exponent, "first_step_probe": first_step_probe, "first_step_address": first_step_address, "first_step_content": first_step_content, "first_step_outgate": first_step_outgate, "first_step_strength_raw": first_step_strength_raw, "channel_scaling_factor": channel_scaling_factor, "readout_projection": readout_projection}


EPSILON = 1e-06
HIGHEST_ACCURACY = lax.Precision.HIGHEST

def unit_inverse(lower_part):
    matrix_order = lower_part.shape[-1]
    identity = jnp.eye(matrix_order, dtype=jnp.float32)
    result = identity - lower_part
    power_term = lower_part
    reached = 2
    while reached < matrix_order:
        power_term = jnp.matmul(power_term, power_term, precision=HIGHEST_ACCURACY)
        result = jnp.matmul(result, identity + power_term, precision=HIGHEST_ACCURACY)
        reached = reached * 2
    return result

def build_arguments(address_vectors, content_vectors, outgate_raw_scores, strength_offset, channel_fading_speed, added_fading_exponent, channel_width):
    length = address_vectors.shape[0]
    attention_channels_total = channel_fading_speed.shape[0]
    address_token_slab = jax.nn.silu(address_vectors.astype(jnp.float32)).reshape(length, attention_channels_total, channel_width)
    address_token_slab = address_token_slab * lax.rsqrt(lax.optimization_barrier(jnp.sum(address_token_slab * address_token_slab, axis=-1, keepdims=True)) + EPSILON)
    content_token_slab = jax.nn.silu(content_vectors.astype(jnp.float32)).reshape(length, attention_channels_total, channel_width)
    strength_raw_expanded = outgate_raw_scores.astype(jnp.float32)
    storing_strength = jax.nn.sigmoid(strength_raw_expanded[:, :attention_channels_total] + strength_offset)
    fading_exponent = added_fading_exponent - channel_fading_speed * jax.nn.softplus(strength_raw_expanded[:, attention_channels_total:])
    return (address_token_slab, content_token_slab, storing_strength, fading_exponent)

def final_state(address_token_slab, content_token_slab, storing_strength, fading_exponent, block):
    length, attention_channels_total, channel_width = address_token_slab.shape
    blocks = length // block

    def split_blocks(tensor):
        moved_axes = jnp.swapaxes(tensor, 0, 1)
        return moved_axes.reshape((attention_channels_total, blocks, block) + moved_axes.shape[2:])
    block_keys = split_blocks(address_token_slab)
    block_values = split_blocks(content_token_slab)
    block_beta = split_blocks(storing_strength)
    cumulative = jnp.cumsum(split_blocks(fading_exponent), axis=-1)
    positions = jnp.arange(block)
    strict = positions[:, None] > positions[None, :]
    spread_log = jnp.where(strict, cumulative[..., :, None] - cumulative[..., None, :], 0.0)
    scaled_keys = block_keys * block_beta[..., None]
    inner_prod = jnp.einsum('hnik,hnjk->hnij', scaled_keys, block_keys, precision=HIGHEST_ACCURACY)
    lower_part = jnp.where(strict, inner_prod * jnp.exp(spread_log), 0.0)
    inverse = unit_inverse(lower_part)
    targets = jnp.concatenate([block_values * block_beta[..., None], scaled_keys * jnp.exp(cumulative)[..., None]], axis=-1)
    solved = jnp.einsum('hnij,hnjk->hnik', inverse, targets, precision=HIGHEST_ACCURACY)
    updates = solved[..., :channel_width]
    key_weights = solved[..., channel_width:]
    tail_keys = block_keys * jnp.exp(cumulative[..., -1:] - cumulative)[..., None]
    last_decay = jnp.exp(cumulative[..., -1])

    def advance(carried_state, block_items):
        update_index, weight_index, tail_index, last_index = block_items
        fresh_value_rows = update_index - jnp.einsum('xbg,xgp->xbp', weight_index, carried_state, precision=HIGHEST_ACCURACY)
        carried_state = carried_state * last_index[:, None, None] + jnp.einsum('tjo,tjw->tow', tail_index, fresh_value_rows, precision=HIGHEST_ACCURACY)
        return (carried_state, None)

    def range_advance(carried_state, range_items):
        carried_state, _ = lax.scan(advance, carried_state, range_items)
        return (carried_state, carried_state)
    blocks_per_range = blocks // RANGES
    initial = jnp.zeros((attention_channels_total, channel_width, channel_width), jnp.float32)
    block_items = (jnp.moveaxis(updates, 1, 0), jnp.moveaxis(key_weights, 1, 0), jnp.moveaxis(tail_keys, 1, 0), jnp.moveaxis(last_decay, 1, 0))
    range_items = tuple((item.reshape((RANGES, blocks_per_range) + item.shape[1:]) for item in block_items))
    _, range_states = lax.scan(range_advance, initial, range_items)
    return range_states

def read_heads(state_cache, first_step_probe, first_step_address, first_step_content, first_step_outgate, first_step_strength_raw, channel_scaling_factor):
    seq_count, attention_channels_total, channel_width, _ = state_cache.shape
    carried_state = state_cache.astype(jnp.float32)

    def activate(tensor):
        return jax.nn.silu(tensor.astype(jnp.float32)).reshape(seq_count, attention_channels_total, channel_width)
    query_rows = activate(first_step_probe)
    address_token_slab = activate(first_step_address)
    address_token_slab = address_token_slab * lax.rsqrt(lax.optimization_barrier(jnp.sum(address_token_slab * address_token_slab, axis=-1, keepdims=True)) + EPSILON)
    content_token_slab = activate(first_step_content)
    storing_strength = jax.nn.sigmoid(first_step_strength_raw)
    recalled = jnp.einsum('nhk,nhkv->nhv', address_token_slab, carried_state, precision=HIGHEST_ACCURACY)
    updated = carried_state + storing_strength[..., None, None] * address_token_slab[..., :, None] * (content_token_slab - recalled)[..., None, :]
    output = jnp.einsum('nhk,nhkv->nhv', query_rows, updated, precision=HIGHEST_ACCURACY)
    normed = output * lax.rsqrt(lax.optimization_barrier(jnp.mean(output * output, axis=-1, keepdims=True)) + EPSILON) * channel_scaling_factor
    gated_out = normed * activate(first_step_outgate)
    return gated_out.reshape(seq_count, attention_channels_total * channel_width).astype(jnp.bfloat16)

def reference(layer_source_tokens, address_projection, content_projection, strength_projection, fading_driver_projection, strength_offset, channel_fading_speed, added_fading_exponent, first_step_probe, first_step_address, first_step_content, first_step_outgate, first_step_strength_raw, channel_scaling_factor, readout_projection):
    seq_count, length, model_width = layer_source_tokens.shape
    flat_rows = layer_source_tokens.reshape(seq_count * length, model_width)

    def product(weight):
        return jnp.dot(flat_rows, weight, preferred_element_type=jnp.float32).astype(jnp.bfloat16)
    address_vectors = product(address_projection).reshape(seq_count, length, -1)
    content_vectors = product(content_projection).reshape(seq_count, length, -1)
    outgate_raw_scores = jnp.concatenate([product(strength_projection), product(fading_driver_projection)], axis=-1).reshape(seq_count, length, -1)

    def solitary_prompt(prompt_members):
        address_token_list, content_token_list, strength_raw_list, prompt_group_tokens = prompt_members
        address_token_slab, content_token_slab, storing_strength, fading_exponent = build_arguments(address_token_list, content_token_list, strength_raw_list, strength_offset, channel_fading_speed, prompt_group_tokens, ADDRESS_WIDTH)
        return final_state(address_token_slab, content_token_slab, storing_strength, fading_exponent, BLOCK)
    range_memories = lax.map(solitary_prompt, (address_vectors, content_vectors, outgate_raw_scores, added_fading_exponent))
    boundary_cache = range_memories.astype(jnp.bfloat16)
    state_cache = range_memories[:, -1].astype(jnp.bfloat16)
    heads_read = read_heads(state_cache, first_step_probe, first_step_address, first_step_content, first_step_outgate, first_step_strength_raw, channel_scaling_factor)
    group_rows = heads_read.astype(jnp.float32).reshape(seq_count, N_TP, -1)
    group_weights = readout_projection.astype(jnp.float32).reshape(N_TP, -1, model_width)
    group_terms = jnp.einsum('stc,tcd->tsd', group_rows, group_weights)
    rounded = lax.optimization_barrier(group_terms.astype(jnp.bfloat16))
    mixed_read = lax.optimization_barrier(jnp.sum(rounded.astype(jnp.float32), axis=0)).astype(jnp.bfloat16)
    return (state_cache, mixed_read, boundary_cache)
```

```python
import jax
import jax.numpy as jnp
from jax import lax
from jax.experimental import pallas as pl
from jax.experimental.pallas import tpu as pltpu
from jax.sharding import PartitionSpec as P

ADDRESS_WIDTH = 128
BLOCK = 64


EPSILON = 1e-06
HIGHEST_ACCURACY = lax.Precision.HIGHEST


def prefix(array, axis, combine, identity):
    peers, index = (lax.axis_size(axis), lax.axis_index(axis))
    everything = jax.tree.map(
        lambda part, kind: lax.all_gather(part.astype(kind), axis),
        array,
        (jnp.bfloat16, jnp.bfloat16),
    )
    start = jax.tree.map(
        lambda part, zero: jnp.broadcast_to(jnp.asarray(zero, part.dtype), part.shape),
        array,
        identity,
    )

    def step(k, before):
        reached = k < index
        new = combine(
            before, jax.tree.map(lambda part, own: part[k].astype(own.dtype), everything, array)
        )
        return jax.tree.map(lambda a, b: jnp.where(reached, a, b), new, before)

    return lax.fori_loop(0, peers, step, start)


def as_sent(array):
    return jax.tree.map(lambda a: a.astype(jnp.bfloat16) if a.dtype == jnp.float32 else a, array)


def broadcast(value, axis, source):
    kept = jnp.where(lax.axis_index(axis) == source, value, 0).astype(value.dtype)
    return lax.psum(kept, axis)


def unit_inverse(lower_part):
    matrix_order = lower_part.shape[-1]
    identity = jnp.eye(matrix_order, dtype=jnp.float32)
    result = identity - lower_part
    power_term = lower_part
    reached = 2
    while reached < matrix_order:
        power_term = jnp.matmul(power_term, power_term, precision=HIGHEST_ACCURACY)
        result = jnp.matmul(result, identity + power_term, precision=HIGHEST_ACCURACY)
        reached = reached * 2
    return result


def build_arguments(
    address_vectors,
    content_vectors,
    outgate_raw_scores,
    strength_offset,
    channel_fading_speed,
    added_fading_exponent,
    channel_width,
):
    length = address_vectors.shape[0]
    attention_channels_total = channel_fading_speed.shape[0]
    address_token_slab = jax.nn.silu(address_vectors.astype(jnp.float32)).reshape(
        length, attention_channels_total, channel_width
    )
    address_token_slab = address_token_slab * lax.rsqrt(
        jnp.sum(address_token_slab * address_token_slab, axis=-1, keepdims=True) + EPSILON
    )
    content_token_slab = jax.nn.silu(content_vectors.astype(jnp.float32)).reshape(
        length, attention_channels_total, channel_width
    )
    strength_raw_expanded = outgate_raw_scores.astype(jnp.float32)
    storing_strength = jax.nn.sigmoid(
        strength_raw_expanded[:, :attention_channels_total] + strength_offset
    )
    fading_exponent = added_fading_exponent - channel_fading_speed * jax.nn.softplus(
        strength_raw_expanded[:, attention_channels_total:]
    )
    return (address_token_slab, content_token_slab, storing_strength, fading_exponent)


def range_map(address_token_slab, content_token_slab, storing_strength, fading_exponent, block):
    length, attention_channels_total, channel_width = address_token_slab.shape
    blocks = length // block

    def split_blocks(tensor):
        moved_axes = jnp.swapaxes(tensor, 0, 1)
        return moved_axes.reshape((attention_channels_total, blocks, block) + moved_axes.shape[2:])

    block_keys = split_blocks(address_token_slab)
    block_values = split_blocks(content_token_slab)
    block_beta = split_blocks(storing_strength)
    cumulative = jnp.cumsum(split_blocks(fading_exponent), axis=-1)
    positions = jnp.arange(block)
    strict = positions[:, None] > positions[None, :]
    spread_log = jnp.where(strict, cumulative[..., :, None] - cumulative[..., None, :], 0.0)
    scaled_keys = block_keys * block_beta[..., None]
    inner_prod = jnp.einsum("hnik,hnjk->hnij", scaled_keys, block_keys, precision=HIGHEST_ACCURACY)
    lower_part = jnp.where(strict, inner_prod * jnp.exp(spread_log), 0.0)
    inverse = unit_inverse(lower_part)
    targets = jnp.concatenate(
        [block_values * block_beta[..., None], scaled_keys * jnp.exp(cumulative)[..., None]],
        axis=-1,
    )
    solved = jnp.einsum("hnij,hnjk->hnik", inverse, targets, precision=HIGHEST_ACCURACY)
    updates = solved[..., :channel_width]
    key_weights = solved[..., channel_width:]
    tail_keys = block_keys * jnp.exp(cumulative[..., -1:] - cumulative)[..., None]
    last_decay = jnp.exp(cumulative[..., -1])
    identity = jnp.eye(channel_width, dtype=jnp.float32)

    def advance(state_pair, block_items):
        transition, carried_state = state_pair
        update_index, weight_index, tail_index, last_index = block_items
        fresh_value_rows = update_index - jnp.einsum(
            "xbg,xgp->xbp", weight_index, carried_state, precision=HIGHEST_ACCURACY
        )
        carried_state = carried_state * last_index[:, None, None] + jnp.einsum(
            "tjo,tjw->tow", tail_index, fresh_value_rows, precision=HIGHEST_ACCURACY
        )
        block_move = last_index[:, None, None] * identity - jnp.einsum(
            "hck,hcj->hkj", tail_index, weight_index, precision=HIGHEST_ACCURACY
        )
        transition = jnp.einsum("hij,hjk->hik", block_move, transition, precision=HIGHEST_ACCURACY)
        return ((transition, carried_state), None)

    initial = (
        jnp.broadcast_to(identity, (attention_channels_total, channel_width, channel_width)),
        jnp.zeros((attention_channels_total, channel_width, channel_width), jnp.float32),
    )
    block_items = (
        jnp.moveaxis(updates, 1, 0),
        jnp.moveaxis(key_weights, 1, 0),
        jnp.moveaxis(tail_keys, 1, 0),
        jnp.moveaxis(last_decay, 1, 0),
    )
    (transition, carried_state), _ = lax.scan(advance, initial, block_items)
    return (transition, carried_state)


def read_heads(
    state_cache,
    first_step_probe,
    first_step_address,
    first_step_content,
    first_step_outgate,
    first_step_strength_raw,
    channel_scaling_factor,
):
    seq_count, attention_channels_total, channel_width, _ = state_cache.shape
    carried_state = state_cache.astype(jnp.float32)

    def activate(tensor):
        return jax.nn.silu(tensor.astype(jnp.float32)).reshape(
            seq_count, attention_channels_total, channel_width
        )

    query_rows = activate(first_step_probe)
    address_token_slab = activate(first_step_address)
    address_token_slab = address_token_slab * lax.rsqrt(
        jnp.sum(address_token_slab * address_token_slab, axis=-1, keepdims=True) + EPSILON
    )
    content_token_slab = activate(first_step_content)
    storing_strength = jax.nn.sigmoid(first_step_strength_raw)
    recalled = jnp.einsum(
        "nhk,nhkv->nhv", address_token_slab, carried_state, precision=HIGHEST_ACCURACY
    )
    updated = (
        carried_state
        + storing_strength[..., None, None]
        * address_token_slab[..., :, None]
        * (content_token_slab - recalled)[..., None, :]
    )
    output = jnp.einsum("nhk,nhkv->nhv", query_rows, updated, precision=HIGHEST_ACCURACY)
    normed = (
        output
        * lax.rsqrt(jnp.mean(output * output, axis=-1, keepdims=True) + EPSILON)
        * channel_scaling_factor
    )
    gated_out = normed * activate(first_step_outgate)
    return gated_out.reshape(seq_count, attention_channels_total * channel_width).astype(
        jnp.bfloat16
    )


def matmul_maps(left, right):
    return jnp.einsum("shij,shjk->shik", left, right, precision=HIGHEST_ACCURACY)


def join_pairs(earlier, later):
    return (matmul_maps(later[0], earlier[0]), matmul_maps(later[0], earlier[1]) + later[1])


def per_device(
    layer_source_tokens,
    address_projection,
    content_projection,
    strength_projection,
    fading_driver_projection,
    strength_offset,
    channel_fading_speed,
    added_fading_exponent,
    first_step_probe,
    first_step_address,
    first_step_content,
    first_step_outgate,
    first_step_strength_raw,
    channel_scaling_factor,
    readout_projection,
):
    head_local = channel_fading_speed.shape[0]
    first_head = lax.axis_index("tp") * head_local
    beta_slice = lax.dynamic_slice_in_dim(strength_projection, first_head, head_local, 1)
    alpha_slice = lax.dynamic_slice_in_dim(fading_driver_projection, first_head, head_local, 1)
    seq_count, local_len, model_width = layer_source_tokens.shape
    flat_rows = layer_source_tokens.reshape(seq_count * local_len, model_width)
    key_sum = jnp.dot(
        flat_rows,
        lax.all_gather(address_projection, "sp", axis=0, tiled=True),
        preferred_element_type=jnp.float32,
    )
    value_sum = jnp.dot(
        flat_rows,
        lax.all_gather(content_projection, "sp", axis=0, tiled=True),
        preferred_element_type=jnp.float32,
    )
    beta_sum = jnp.dot(flat_rows, beta_slice, preferred_element_type=jnp.float32)
    alpha_sum = jnp.dot(flat_rows, alpha_slice, preferred_element_type=jnp.float32)
    outgate_raw_scores = (
        jnp.concatenate([beta_sum, alpha_sum], axis=1)
        .astype(jnp.bfloat16)
        .reshape(seq_count, local_len, -1)
    )
    address_vectors = key_sum.astype(jnp.bfloat16).reshape(seq_count, local_len, -1)
    content_vectors = value_sum.astype(jnp.bfloat16).reshape(seq_count, local_len, -1)
    transitions = []
    offsets = []
    for prompt_number in range(seq_count):
        address_token_slab, content_token_slab, storing_strength, fading_exponent = build_arguments(
            address_vectors[prompt_number],
            content_vectors[prompt_number],
            outgate_raw_scores[prompt_number],
            strength_offset,
            channel_fading_speed,
            added_fading_exponent[prompt_number],
            ADDRESS_WIDTH,
        )
        transition, carried_state = range_map(
            address_token_slab, content_token_slab, storing_strength, fading_exponent, BLOCK
        )
        transitions.append(transition)
        offsets.append(carried_state)
    transition = jnp.stack(transitions)
    offset = jnp.stack(offsets)
    identity = jnp.broadcast_to(jnp.eye(ADDRESS_WIDTH, dtype=jnp.float32), transition.shape)
    entered = prefix((transition, offset), "sp", join_pairs, (identity, jnp.zeros_like(offset)))
    leaving = matmul_maps(transition, entered[1]) + offset
    final = broadcast(as_sent(leaving), "sp", lax.axis_size("sp") - 1).astype(leaving.dtype)
    boundary_cache = leaving.astype(jnp.bfloat16)[:, None]
    state_cache = final.astype(jnp.bfloat16)
    heads_read = read_heads(
        state_cache,
        first_step_probe,
        first_step_address,
        first_step_content,
        first_step_outgate,
        first_step_strength_raw,
        channel_scaling_factor,
    )
    group_terms = jnp.dot(
        heads_read, readout_projection, preferred_element_type=jnp.float32
    ).astype(jnp.bfloat16)
    mixed_read = lax.psum(group_terms.astype(jnp.float32).astype(jnp.bfloat16), "tp")
    return (state_cache, mixed_read, boundary_cache)


MESH = pl.DeviceIdType.MESH
PIECES = 2


def remote(src, dst, send, recv, sp, tp):
    return pltpu.make_async_remote_copy(
        src_ref=src,
        dst_ref=dst,
        send_sem=send,
        recv_sem=recv,
        device_id={"sp": sp, "tp": tp},
        device_id_type=MESH,
    )


def gather_kernel(
    peers,
    tok,
    wk,
    wv,
    add,
    xall,
    wall,
    addall,
    own_sem,
    across_send,
    a_send,
    b_send,
    tok_recv,
    w_send,
    w_recv,
    relay_send,
    relay_recv,
    add_send,
    add_recv,
):
    s, t = lax.axis_index("sp"), lax.axis_index("tp")
    ring = peers // 2
    x, q = s % 2, s // 2
    half = tok.shape[2] // 2
    length = tok.shape[1]
    piece = length // PIECES
    rows = wk.shape[0]
    width = ADDRESS_WIDTH
    columns = pl.ds(pl.multiple_of(t * half, 128), half)

    def place(r):
        y = r // (ring // 2)
        z = (1 - y) * r + y * (ring - 1 - r)
        return 2 * z + y

    y, z = q % 2, q // 2
    r = (1 - y) * z + y * (ring - 1 - z)
    after = place((r + 1) % ring)
    before = place((r + ring - 1) % ring)

    def part(i):
        return pl.ds(i * piece, piece)

    def token_wait(slot, i):
        ref = xall.at[slot, part(i)]
        remote(ref, ref, across_send.at[i], tok_recv.at[slot, i], s, t).wait_recv()

    sent = []

    def go(copy):
        copy.start()
        sent.append(copy)

    for i in range(PIECES):
        go(
            remote(
                tok.at[1 - x, part(i), columns],
                xall.at[s, part(i)],
                across_send.at[i],
                tok_recv.at[s, i],
                2 * q + 1 - x,
                t,
            )
        )
        go(
            remote(
                tok.at[x, part(i), columns],
                xall.at[s, part(i)],
                a_send.at[0, i],
                tok_recv.at[s, i],
                2 * after + x,
                t,
            )
        )
    own = pltpu.make_async_copy(tok.at[x, :, columns], xall.at[s], own_sem)
    own.start()

    side = s // ring
    row_slot = s % ring
    spot = pl.ds(pl.multiple_of(row_slot * rows, 16), rows)
    for off in range(ring):
        head = (q + off) % ring
        for kv, w in enumerate((wk, wv)):
            src = w.at[:, pl.ds(pl.multiple_of(head * width, 128), width)]
            dst = wall.at[spot, pl.ds(pl.multiple_of((2 * t + kv) * width, 128), width)]
            copy = remote(
                src, dst, w_send.at[off, kv], w_recv.at[row_slot, 2 * t + kv], 2 * head + x, side
            )
            if off == 0:

                @pl.when(t == side)
                def _():
                    pltpu.make_async_copy(src, dst, w_recv.at[row_slot, 2 * t + kv]).start()

                @pl.when(t != side)
                def _():
                    copy.start()
            else:
                go(copy)

    for off in range(1, peers):
        to = (s + off) % peers
        go(remote(add.at[to % 2], addall.at[s], add_send.at[off], add_recv.at[s], to, t))
    own_add = pltpu.make_async_copy(add.at[x], addall.at[s], add_recv.at[s])
    own_add.start()

    def relay(m):
        slot = 2 * m + x
        block = wall.at[pl.ds(pl.multiple_of(slot * rows, 16), rows)]
        for c in range(4):
            one = wall.at[pl.ds(pl.multiple_of(slot * rows, 16), rows), pl.ds(c * width, width)]
            pltpu.make_async_copy(one, one, w_recv.at[slot, c]).wait()
        go(remote(block, block, relay_send.at[m], relay_recv.at[slot], 2 * q + 1 - x, t))

    relays = list(range(ring // 2))
    for k in range(ring - 1):
        for i in range(PIECES):
            if k > 0:
                slot = 2 * place((r - k + ring) % ring) + x
                token_wait(slot, i)
                ref = xall.at[slot, part(i)]
                go(remote(ref, ref, a_send.at[k, i], tok_recv.at[slot, i], 2 * after + x, t))
            slot = 2 * place((r + k) % ring) + 1 - x
            token_wait(slot, i)
            ref = xall.at[slot, part(i)]
            go(remote(ref, ref, b_send.at[k, i], tok_recv.at[slot, i], 2 * before + x, t))
        if k >= 2 and relays:
            relay(relays.pop(0))
    while relays:
        relay(relays.pop(0))
    for i in range(PIECES):
        token_wait(2 * place((r + 1) % ring) + x, i)
        token_wait(2 * place((r + ring - 1) % ring) + 1 - x, i)
    for m in range(ring // 2):
        slot = 2 * m + 1 - x
        block = wall.at[pl.ds(pl.multiple_of(slot * rows, 16), rows)]
        remote(block, block, relay_send.at[m], relay_recv.at[slot], s, t).wait_recv()
    own.wait()
    for off in range(peers):
        slot = (s + off) % peers
        pltpu.make_async_copy(addall.at[slot], addall.at[slot], add_recv.at[slot]).wait()
    for copy in sent:
        copy.wait_send()

    @pl.when(t != side)
    def _():
        for kv, w in enumerate((wk, wv)):
            src = w.at[:, pl.ds(pl.multiple_of(q * width, 128), width)]
            dst = wall.at[spot, pl.ds(pl.multiple_of((2 * t + kv) * width, 128), width)]
            remote(
                src, dst, w_send.at[0, kv], w_recv.at[row_slot, 2 * t + kv], 2 * q + x, side
            ).wait_send()


def gather_inputs(tok, wk, wv, add, peers):
    seq_count, length, model_width = tok.shape
    ring = peers // 2
    heads = add.shape[1]
    dma = pltpu.SemaphoreType.DMA
    anywhere = pl.BlockSpec(memory_space=pl.ANY)
    vmem = pl.BlockSpec(memory_space=pltpu.VMEM)
    return pl.pallas_call(
        lambda *refs: gather_kernel(peers, *refs),
        out_shape=(
            jax.ShapeDtypeStruct((peers, length, model_width // 2), tok.dtype),
            jax.ShapeDtypeStruct((model_width // 2, 4 * ADDRESS_WIDTH), wk.dtype),
            jax.ShapeDtypeStruct((peers, heads, length), add.dtype),
        ),
        in_specs=[anywhere] * 4,
        out_specs=(vmem, vmem, vmem),
        scratch_shapes=[
            dma(()),
            dma((PIECES,)),
            dma((ring - 1, PIECES)),
            dma((ring - 1, PIECES)),
            dma((peers, PIECES)),
            dma((ring, 2)),
            dma((ring, 4)),
            dma((ring // 2,)),
            dma((ring,)),
            dma((peers,)),
            dma((peers,)),
        ],
        compiler_params=pltpu.CompilerParams(has_side_effects=True),
        name="gather_inputs",
    )(tok, wk, wv, add)


def spread_kernel(peers, states, final, bound, f_send, f_recv, b_send, b_recv):
    s, t = lax.axis_index("sp"), lax.axis_index("tp")
    ring = peers // 2
    slot = (s % 2) * ring + s // 2
    sent = []
    for send, recv, out, last in ((f_send, f_recv, final, True), (b_send, b_recv, bound, False)):
        for off in range(1, peers):
            to = (s + off) % peers
            copy = remote(
                states.at[peers - 1 if last else to],
                out.at[slot],
                send.at[off],
                recv.at[slot],
                to,
                t,
            )
            copy.start()
            sent.append(copy)
    final[slot] = states[peers - 1]
    bound[slot] = states[s]
    for out, recv in ((final, f_recv), (bound, b_recv)):
        for off in range(1, peers):
            other = (s + off) % peers
            slot_from = (other % 2) * ring + other // 2
            ref = out.at[slot_from]
            remote(ref, ref, f_send.at[off], recv.at[slot_from], s, t).wait_recv()
    for copy in sent:
        copy.wait_send()


def spread_states(states, peers):
    dma = pltpu.SemaphoreType.DMA
    vmem = pl.BlockSpec(memory_space=pltpu.VMEM)
    return pl.pallas_call(
        lambda *refs: spread_kernel(peers, *refs),
        out_shape=(jax.ShapeDtypeStruct(states.shape, states.dtype),) * 2,
        in_specs=[vmem],
        out_specs=(vmem, vmem),
        scratch_shapes=[dma((peers,))] * 4,
        compiler_params=pltpu.CompilerParams(has_side_effects=True),
        name="spread_states",
    )(states)


def dot32(spec, a, b):
    return jnp.einsum(spec, a, b, precision=HIGHEST_ACCURACY)


def block_states(keys, values, beta, fading):
    blocks, block, width = keys.shape
    cumulative = jnp.cumsum(fading, axis=-1)
    positions = jnp.arange(block)
    strict = positions[:, None] > positions[None, :]
    spread_log = jnp.where(strict, cumulative[:, :, None] - cumulative[:, None, :], 0.0)
    scaled_keys = keys * beta[..., None]
    inner = dot32("nik,njk->nij", scaled_keys, keys)
    inverse = unit_inverse(jnp.where(strict, inner * jnp.exp(spread_log), 0.0))
    targets = jnp.concatenate(
        [scaled_keys * jnp.exp(cumulative)[..., None], values * beta[..., None]], axis=-1
    )
    solved = dot32("nij,njk->nik", inverse, targets)
    tail = keys * jnp.exp(cumulative[:, -1:] - cumulative)[..., None]
    maps = dot32("nck,ncj->nkj", tail, solved)
    last = jnp.exp(cumulative[:, -1])[:, None, None]
    moves = last * jnp.eye(width, dtype=jnp.float32) - maps[..., :width]
    pair = jnp.concatenate([moves, maps[..., width:]], axis=-1)
    zero = jnp.zeros((blocks, width, width), jnp.float32)
    reach = 1
    while reach < blocks:
        late = pair[reach:]
        joined = dot32("nij,njk->nik", late[..., :width], pair[:-reach])
        joined = joined + jnp.concatenate([zero[reach:], late[..., width:]], axis=-1)
        pair = jnp.concatenate([pair[:reach], joined], axis=0)
        reach *= 2
    return pair[..., width:]


def per_device_heads(
    layer_source_tokens,
    address_projection,
    content_projection,
    strength_projection,
    fading_driver_projection,
    strength_offset,
    channel_fading_speed,
    added_fading_exponent,
    first_step_probe,
    first_step_address,
    first_step_content,
    first_step_outgate,
    first_step_strength_raw,
    channel_scaling_factor,
    readout_projection,
):
    peers = lax.axis_size("sp")
    head_local = channel_fading_speed.shape[0]
    s, t = lax.axis_index("sp"), lax.axis_index("tp")
    mine = s // 2
    _, length, model_width = layer_source_tokens.shape
    half = model_width // 2
    width = ADDRESS_WIDTH
    tokens, weights, added = gather_inputs(
        layer_source_tokens,
        address_projection,
        content_projection,
        jnp.swapaxes(added_fading_exponent, 1, 2),
        peers,
    )
    flat = tokens.reshape(peers * length, half)
    gates = jnp.concatenate([strength_projection, fading_driver_projection], axis=1)
    gates = lax.dynamic_slice_in_dim(gates, t * half, half, 0)
    wide = jnp.dot(flat, weights, preferred_element_type=jnp.float32)
    gate_sum = jnp.dot(flat, gates, preferred_element_type=jnp.float32)
    gate_sum = lax.psum(gate_sum, "tp").astype(jnp.bfloat16).astype(jnp.float32)
    kept = lax.dynamic_slice_in_dim(wide, t * 2 * width, 2 * width, 1)
    given = lax.dynamic_slice_in_dim(wide, (1 - t) * 2 * width, 2 * width, 1)
    wide = kept + lax.ppermute(given, "tp", ((0, 1), (1, 0)))
    wide = wide.astype(jnp.bfloat16).astype(jnp.float32).reshape(peers, length, 2 * width)
    acted = jax.nn.silu(wide)
    keys = acted[..., :width]
    keys = keys * lax.rsqrt(jnp.sum(keys * keys, axis=-1, keepdims=True) + EPSILON)
    values = acted[..., width:]
    head = t * head_local + mine
    total_heads = strength_projection.shape[1]
    beta_logit = lax.dynamic_slice_in_dim(gate_sum, head, 1, 1).reshape(peers, length)
    alpha_logit = lax.dynamic_slice_in_dim(gate_sum, total_heads + head, 1, 1).reshape(
        peers, length
    )
    beta = jax.nn.sigmoid(beta_logit + lax.dynamic_index_in_dim(strength_offset, mine, 0))
    added_own = lax.dynamic_index_in_dim(added, mine, 1, keepdims=False)
    speed = lax.dynamic_index_in_dim(channel_fading_speed, mine, 0)
    fading = added_own - speed * jax.nn.softplus(alpha_logit)
    states = block_states(keys, values, beta, fading).astype(jnp.bfloat16)
    final, bound = spread_states(states, peers)
    state_cache = final.reshape(2, head_local, width, width)
    boundary_cache = bound.reshape(2, 1, head_local, width, width)
    heads_read = read_heads(
        state_cache,
        first_step_probe,
        first_step_address,
        first_step_content,
        first_step_outgate,
        first_step_strength_raw,
        channel_scaling_factor,
    )
    group_terms = jnp.dot(
        heads_read, readout_projection, preferred_element_type=jnp.float32
    ).astype(jnp.bfloat16)
    return (state_cache, lax.psum(group_terms, "tp"), boundary_cache)


def by_heads(mesh):
    def choose(*args):
        seq_count, length, model_width = args[0].shape
        peers, heads = lax.axis_size("sp"), args[6].shape[0]
        fits = (
            lax.axis_size("tp") == 2
            and seq_count == 2
            and peers == 2 * heads
            and heads % 2 == 0
            and length == BLOCK
            and args[1].shape[0] * peers == model_width
        )
        return per_device_heads(*args) if fits else per_device(*args)

    return choose


def solution(mesh):
    return jax.shard_map(
        by_heads(mesh),
        mesh=mesh,
        in_specs=(
            P(None, "sp", None),
            P("sp", "tp"),
            P("sp", "tp"),
            P(),
            P(),
            P("tp"),
            P("tp"),
            P(None, "sp", "tp"),
            P(None, "tp"),
            P(None, "tp"),
            P(None, "tp"),
            P(None, "tp"),
            P(None, "tp"),
            P(),
            P("tp", "sp"),
        ),
        out_specs=(P(None, "tp", None, None), P(None, "sp"), P(None, "sp", "tp", None, None)),
        check_vma=False,
    )
```

```python
import jax
import jax.numpy as jnp
from jax import lax
from jax.experimental import pallas as pl
from jax.experimental.pallas import tpu as pltpu
from jax.sharding import PartitionSpec as P

ADDRESS_WIDTH = 128
BLOCK = 64


EPSILON = 1e-06
HIGHEST_ACCURACY = lax.Precision.HIGHEST


def prefix(array, axis, combine, identity):
    peers, index = (lax.axis_size(axis), lax.axis_index(axis))
    everything = jax.tree.map(
        lambda part, kind: lax.all_gather(part.astype(kind), axis),
        array,
        (jnp.bfloat16, jnp.bfloat16),
    )
    start = jax.tree.map(
        lambda part, zero: jnp.broadcast_to(jnp.asarray(zero, part.dtype), part.shape),
        array,
        identity,
    )

    def step(k, before):
        reached = k < index
        new = combine(
            before, jax.tree.map(lambda part, own: part[k].astype(own.dtype), everything, array)
        )
        return jax.tree.map(lambda a, b: jnp.where(reached, a, b), new, before)

    return lax.fori_loop(0, peers, step, start)


def as_sent(array):
    return jax.tree.map(lambda a: a.astype(jnp.bfloat16) if a.dtype == jnp.float32 else a, array)


def broadcast(value, axis, source):
    kept = jnp.where(lax.axis_index(axis) == source, value, 0).astype(value.dtype)
    return lax.psum(kept, axis)


def unit_inverse(lower_part):
    matrix_order = lower_part.shape[-1]
    identity = jnp.eye(matrix_order, dtype=jnp.float32)
    result = identity - lower_part
    power_term = lower_part
    reached = 2
    while reached < matrix_order:
        power_term = jnp.matmul(power_term, power_term, precision=HIGHEST_ACCURACY)
        result = jnp.matmul(result, identity + power_term, precision=HIGHEST_ACCURACY)
        reached = reached * 2
    return result


def build_arguments(
    address_vectors,
    content_vectors,
    outgate_raw_scores,
    strength_offset,
    channel_fading_speed,
    added_fading_exponent,
    channel_width,
):
    length = address_vectors.shape[0]
    attention_channels_total = channel_fading_speed.shape[0]
    address_token_slab = jax.nn.silu(address_vectors.astype(jnp.float32)).reshape(
        length, attention_channels_total, channel_width
    )
    address_token_slab = address_token_slab * lax.rsqrt(
        jnp.sum(address_token_slab * address_token_slab, axis=-1, keepdims=True) + EPSILON
    )
    content_token_slab = jax.nn.silu(content_vectors.astype(jnp.float32)).reshape(
        length, attention_channels_total, channel_width
    )
    strength_raw_expanded = outgate_raw_scores.astype(jnp.float32)
    storing_strength = jax.nn.sigmoid(
        strength_raw_expanded[:, :attention_channels_total] + strength_offset
    )
    fading_exponent = added_fading_exponent - channel_fading_speed * jax.nn.softplus(
        strength_raw_expanded[:, attention_channels_total:]
    )
    return (address_token_slab, content_token_slab, storing_strength, fading_exponent)


def range_map(address_token_slab, content_token_slab, storing_strength, fading_exponent, block):
    length, attention_channels_total, channel_width = address_token_slab.shape
    blocks = length // block

    def split_blocks(tensor):
        moved_axes = jnp.swapaxes(tensor, 0, 1)
        return moved_axes.reshape((attention_channels_total, blocks, block) + moved_axes.shape[2:])

    block_keys = split_blocks(address_token_slab)
    block_values = split_blocks(content_token_slab)
    block_beta = split_blocks(storing_strength)
    cumulative = jnp.cumsum(split_blocks(fading_exponent), axis=-1)
    positions = jnp.arange(block)
    strict = positions[:, None] > positions[None, :]
    spread_log = jnp.where(strict, cumulative[..., :, None] - cumulative[..., None, :], 0.0)
    scaled_keys = block_keys * block_beta[..., None]
    inner_prod = jnp.einsum("hnik,hnjk->hnij", scaled_keys, block_keys, precision=HIGHEST_ACCURACY)
    lower_part = jnp.where(strict, inner_prod * jnp.exp(spread_log), 0.0)
    inverse = unit_inverse(lower_part)
    targets = jnp.concatenate(
        [block_values * block_beta[..., None], scaled_keys * jnp.exp(cumulative)[..., None]],
        axis=-1,
    )
    solved = jnp.einsum("hnij,hnjk->hnik", inverse, targets, precision=HIGHEST_ACCURACY)
    updates = solved[..., :channel_width]
    key_weights = solved[..., channel_width:]
    tail_keys = block_keys * jnp.exp(cumulative[..., -1:] - cumulative)[..., None]
    last_decay = jnp.exp(cumulative[..., -1])
    identity = jnp.eye(channel_width, dtype=jnp.float32)

    def advance(state_pair, block_items):
        transition, carried_state = state_pair
        update_index, weight_index, tail_index, last_index = block_items
        fresh_value_rows = update_index - jnp.einsum(
            "xbg,xgp->xbp", weight_index, carried_state, precision=HIGHEST_ACCURACY
        )
        carried_state = carried_state * last_index[:, None, None] + jnp.einsum(
            "tjo,tjw->tow", tail_index, fresh_value_rows, precision=HIGHEST_ACCURACY
        )
        block_move = last_index[:, None, None] * identity - jnp.einsum(
            "hck,hcj->hkj", tail_index, weight_index, precision=HIGHEST_ACCURACY
        )
        transition = jnp.einsum("hij,hjk->hik", block_move, transition, precision=HIGHEST_ACCURACY)
        return ((transition, carried_state), None)

    initial = (
        jnp.broadcast_to(identity, (attention_channels_total, channel_width, channel_width)),
        jnp.zeros((attention_channels_total, channel_width, channel_width), jnp.float32),
    )
    block_items = (
        jnp.moveaxis(updates, 1, 0),
        jnp.moveaxis(key_weights, 1, 0),
        jnp.moveaxis(tail_keys, 1, 0),
        jnp.moveaxis(last_decay, 1, 0),
    )
    (transition, carried_state), _ = lax.scan(advance, initial, block_items)
    return (transition, carried_state)


def read_heads(
    state_cache,
    first_step_probe,
    first_step_address,
    first_step_content,
    first_step_outgate,
    first_step_strength_raw,
    channel_scaling_factor,
):
    seq_count, attention_channels_total, channel_width, _ = state_cache.shape
    carried_state = state_cache.astype(jnp.float32)

    def activate(tensor):
        return jax.nn.silu(tensor.astype(jnp.float32)).reshape(
            seq_count, attention_channels_total, channel_width
        )

    query_rows = activate(first_step_probe)
    address_token_slab = activate(first_step_address)
    address_token_slab = address_token_slab * lax.rsqrt(
        jnp.sum(address_token_slab * address_token_slab, axis=-1, keepdims=True) + EPSILON
    )
    content_token_slab = activate(first_step_content)
    storing_strength = jax.nn.sigmoid(first_step_strength_raw)
    recalled = jnp.einsum(
        "nhk,nhkv->nhv", address_token_slab, carried_state, precision=HIGHEST_ACCURACY
    )
    updated = (
        carried_state
        + storing_strength[..., None, None]
        * address_token_slab[..., :, None]
        * (content_token_slab - recalled)[..., None, :]
    )
    output = jnp.einsum("nhk,nhkv->nhv", query_rows, updated, precision=HIGHEST_ACCURACY)
    normed = (
        output
        * lax.rsqrt(jnp.mean(output * output, axis=-1, keepdims=True) + EPSILON)
        * channel_scaling_factor
    )
    gated_out = normed * activate(first_step_outgate)
    return gated_out.reshape(seq_count, attention_channels_total * channel_width).astype(
        jnp.bfloat16
    )


def matmul_maps(left, right):
    return jnp.einsum("shij,shjk->shik", left, right, precision=HIGHEST_ACCURACY)


def join_pairs(earlier, later):
    return (matmul_maps(later[0], earlier[0]), matmul_maps(later[0], earlier[1]) + later[1])


def per_device(
    layer_source_tokens,
    address_projection,
    content_projection,
    strength_projection,
    fading_driver_projection,
    strength_offset,
    channel_fading_speed,
    added_fading_exponent,
    first_step_probe,
    first_step_address,
    first_step_content,
    first_step_outgate,
    first_step_strength_raw,
    channel_scaling_factor,
    readout_projection,
):
    head_local = channel_fading_speed.shape[0]
    first_head = lax.axis_index("tp") * head_local
    beta_slice = lax.dynamic_slice_in_dim(strength_projection, first_head, head_local, 1)
    alpha_slice = lax.dynamic_slice_in_dim(fading_driver_projection, first_head, head_local, 1)
    seq_count, local_len, model_width = layer_source_tokens.shape
    flat_rows = layer_source_tokens.reshape(seq_count * local_len, model_width)
    key_sum = jnp.dot(
        flat_rows,
        lax.all_gather(address_projection, "sp", axis=0, tiled=True),
        preferred_element_type=jnp.float32,
    )
    value_sum = jnp.dot(
        flat_rows,
        lax.all_gather(content_projection, "sp", axis=0, tiled=True),
        preferred_element_type=jnp.float32,
    )
    beta_sum = jnp.dot(flat_rows, beta_slice, preferred_element_type=jnp.float32)
    alpha_sum = jnp.dot(flat_rows, alpha_slice, preferred_element_type=jnp.float32)
    outgate_raw_scores = (
        jnp.concatenate([beta_sum, alpha_sum], axis=1)
        .astype(jnp.bfloat16)
        .reshape(seq_count, local_len, -1)
    )
    address_vectors = key_sum.astype(jnp.bfloat16).reshape(seq_count, local_len, -1)
    content_vectors = value_sum.astype(jnp.bfloat16).reshape(seq_count, local_len, -1)
    transitions = []
    offsets = []
    for prompt_number in range(seq_count):
        address_token_slab, content_token_slab, storing_strength, fading_exponent = build_arguments(
            address_vectors[prompt_number],
            content_vectors[prompt_number],
            outgate_raw_scores[prompt_number],
            strength_offset,
            channel_fading_speed,
            added_fading_exponent[prompt_number],
            ADDRESS_WIDTH,
        )
        transition, carried_state = range_map(
            address_token_slab, content_token_slab, storing_strength, fading_exponent, BLOCK
        )
        transitions.append(transition)
        offsets.append(carried_state)
    transition = jnp.stack(transitions)
    offset = jnp.stack(offsets)
    identity = jnp.broadcast_to(jnp.eye(ADDRESS_WIDTH, dtype=jnp.float32), transition.shape)
    entered = prefix((transition, offset), "sp", join_pairs, (identity, jnp.zeros_like(offset)))
    leaving = matmul_maps(transition, entered[1]) + offset
    final = broadcast(as_sent(leaving), "sp", lax.axis_size("sp") - 1).astype(leaving.dtype)
    boundary_cache = leaving.astype(jnp.bfloat16)[:, None]
    state_cache = final.astype(jnp.bfloat16)
    heads_read = read_heads(
        state_cache,
        first_step_probe,
        first_step_address,
        first_step_content,
        first_step_outgate,
        first_step_strength_raw,
        channel_scaling_factor,
    )
    group_terms = jnp.dot(
        heads_read, readout_projection, preferred_element_type=jnp.float32
    ).astype(jnp.bfloat16)
    mixed_read = lax.psum(group_terms.astype(jnp.float32).astype(jnp.bfloat16), "tp")
    return (state_cache, mixed_read, boundary_cache)


MESH = pl.DeviceIdType.MESH
PIECES = 2


def remote(src, dst, send, recv, sp, tp):
    return pltpu.make_async_remote_copy(
        src_ref=src,
        dst_ref=dst,
        send_sem=send,
        recv_sem=recv,
        device_id={"sp": sp, "tp": tp},
        device_id_type=MESH,
    )


def gather_kernel(
    peers,
    tok,
    wk,
    wv,
    add,
    gates,
    out,
    addall,
    xall,
    wall,
    keep,
    give,
    got,
    own_sem,
    across_send,
    a_send,
    b_send,
    tok_recv,
    w_send,
    w_recv,
    relay_send,
    relay_recv,
    add_send,
    add_recv,
    give_send,
    give_recv,
):
    s, t = lax.axis_index("sp"), lax.axis_index("tp")
    ring = peers // 2
    x, q = s % 2, s // 2
    half = tok.shape[2] // 2
    length = tok.shape[1]
    piece = length // PIECES
    rows = wk.shape[0]
    width = ADDRESS_WIDTH
    columns = pl.ds(pl.multiple_of(t * half, 128), half)

    def place(r):
        y = r // (ring // 2)
        z = (1 - y) * r + y * (ring - 1 - r)
        return 2 * z + y

    y, z = q % 2, q // 2
    r = (1 - y) * z + y * (ring - 1 - z)
    after = place((r + 1) % ring)
    before = place((r + ring - 1) % ring)

    def part(i):
        return pl.ds(i * piece, piece)

    def token_wait(slot, i):
        ref = xall.at[slot, part(i)]
        remote(ref, ref, across_send.at[i], tok_recv.at[slot, i], s, t).wait_recv()

    sent = []

    def go(copy):
        copy.start()
        sent.append(copy)

    for i in range(PIECES):
        go(
            remote(
                tok.at[1 - x, part(i), columns],
                xall.at[s, part(i)],
                across_send.at[i],
                tok_recv.at[s, i],
                2 * q + 1 - x,
                t,
            )
        )
        go(
            remote(
                tok.at[x, part(i), columns],
                xall.at[s, part(i)],
                a_send.at[0, i],
                tok_recv.at[s, i],
                2 * after + x,
                t,
            )
        )
    own = pltpu.make_async_copy(tok.at[x, :, columns], xall.at[s], own_sem)
    own.start()

    side = s // ring
    other = (t + side) % 2
    row_slot = s % ring
    spot = pl.ds(pl.multiple_of(row_slot * rows, 16), rows)
    for off in range(ring):
        head = (q + off) % ring
        for kv, w in enumerate((wk, wv)):
            src = w.at[:, pl.ds(pl.multiple_of(head * width, 128), width)]
            dst = wall.at[spot, pl.ds(pl.multiple_of((2 * other + kv) * width, 128), width)]
            copy = remote(
                src, dst, w_send.at[off, kv], w_recv.at[row_slot, 2 * other + kv], 2 * head + x, side
            )
            if off == 0:

                @pl.when(t == side)
                def _():
                    pltpu.make_async_copy(src, dst, w_recv.at[row_slot, 2 * other + kv]).start()

                @pl.when(t != side)
                def _():
                    copy.start()
            else:
                go(copy)

    for off in range(1, peers):
        to = (s + off) % peers
        go(remote(add.at[to % 2], addall.at[s], add_send.at[off], add_recv.at[s], to, t))
    own_add = pltpu.make_async_copy(add.at[x], addall.at[s], add_recv.at[s])
    own_add.start()

    def relay(m):
        slot = 2 * m + x
        block = wall.at[pl.ds(pl.multiple_of(slot * rows, 16), rows)]
        for c in range(4):
            one = wall.at[pl.ds(pl.multiple_of(slot * rows, 16), rows), pl.ds(c * width, width)]
            pltpu.make_async_copy(one, one, w_recv.at[slot, c]).wait()
        go(remote(block, block, relay_send.at[m], relay_recv.at[slot], 2 * q + 1 - x, t))

    relays = list(range(ring // 2))
    for k in range(ring - 1):
        for i in range(PIECES):
            if k > 0:
                slot = 2 * place((r - k + ring) % ring) + x
                token_wait(slot, i)
                ref = xall.at[slot, part(i)]
                go(remote(ref, ref, a_send.at[k, i], tok_recv.at[slot, i], 2 * after + x, t))
            slot = 2 * place((r + k) % ring) + 1 - x
            token_wait(slot, i)
            ref = xall.at[slot, part(i)]
            go(remote(ref, ref, b_send.at[k, i], tok_recv.at[slot, i], 2 * before + x, t))
        if k >= 2 and relays:
            relay(relays.pop(0))
    while relays:
        relay(relays.pop(0))
    for m in range(ring // 2):
        slot = 2 * m + 1 - x
        block = wall.at[pl.ds(pl.multiple_of(slot * rows, 16), rows)]
        remote(block, block, relay_send.at[m], relay_recv.at[slot], s, t).wait_recv()
    own.wait()

    def project(g):
        slots = []
        for k in (2 * g, 2 * g + 1):
            slots.append(2 * place((r - k + ring) % ring) + x)
            slots.append(2 * place((r + k) % ring) + 1 - x)
        rows_in = jnp.concatenate([xall[slot] for slot in slots], axis=0)
        wide = jnp.dot(rows_in, wall[...], preferred_element_type=jnp.float32)
        logits = jnp.dot(rows_in, gates[...], preferred_element_type=jnp.float32)
        for i, slot in enumerate(slots):
            part_of = slice(i * length, (i + 1) * length)
            keep[slot, :, : 2 * width] = wide[part_of, : 2 * width]
            keep[slot, :, 2 * width :] = logits[part_of]
            give[slot, :, : 2 * width] = wide[part_of, 2 * width :]
            give[slot, :, 2 * width :] = logits[part_of]
        for slot in slots:
            remote(
                give.at[slot], got.at[slot], give_send.at[slot], give_recv.at[slot], s, 1 - t
            ).start()

    lax.fori_loop(0, ring // 2 - 1, lambda g, c: (project(g), c)[1], 0)
    for i in range(PIECES):
        token_wait(2 * place((r + 1) % ring) + x, i)
        token_wait(2 * place((r + ring - 1) % ring) + 1 - x, i)
    project(ring // 2 - 1)
    for off in range(peers):
        slot = (s + off) % peers
        pltpu.make_async_copy(addall.at[slot], addall.at[slot], add_recv.at[slot]).wait()
    for copy in sent:
        copy.wait_send()

    def finish(slot, c):
        copy = remote(
            give.at[slot], got.at[slot], give_send.at[slot], give_recv.at[slot], s, 1 - t
        )
        copy.wait_recv()
        out[slot] = (keep[slot] + got[slot]).astype(out.dtype)
        copy.wait_send()
        return c

    lax.fori_loop(0, peers, finish, 0)

    @pl.when(t != side)
    def _():
        for kv, w in enumerate((wk, wv)):
            src = w.at[:, pl.ds(pl.multiple_of(q * width, 128), width)]
            dst = wall.at[spot, pl.ds(pl.multiple_of((2 * other + kv) * width, 128), width)]
            remote(
                src, dst, w_send.at[0, kv], w_recv.at[row_slot, 2 * other + kv], 2 * q + x, side
            ).wait_send()


def gather_inputs(tok, wk, wv, add, gates, peers):
    seq_count, length, model_width = tok.shape
    ring = peers // 2
    heads = add.shape[1]
    dma = pltpu.SemaphoreType.DMA
    anywhere = pl.BlockSpec(memory_space=pl.ANY)
    vmem = pl.BlockSpec(memory_space=pltpu.VMEM)
    return pl.pallas_call(
        lambda *refs: gather_kernel(peers, *refs),
        out_shape=(
            jax.ShapeDtypeStruct((peers, length, 2 * ADDRESS_WIDTH + gates.shape[1]), tok.dtype),
            jax.ShapeDtypeStruct((peers, heads, length), add.dtype),
        ),
        in_specs=[anywhere] * 4 + [vmem],
        out_specs=(vmem, vmem),
        scratch_shapes=[
            pltpu.VMEM((peers, length, model_width // 2), tok.dtype),
            pltpu.VMEM((model_width // 2, 4 * ADDRESS_WIDTH), wk.dtype),
            pltpu.VMEM((peers, length, 2 * ADDRESS_WIDTH + gates.shape[1]), jnp.float32),
            pltpu.VMEM((peers, length, 2 * ADDRESS_WIDTH + gates.shape[1]), jnp.float32),
            pltpu.VMEM((peers, length, 2 * ADDRESS_WIDTH + gates.shape[1]), jnp.float32),
            dma(()),
            dma((PIECES,)),
            dma((ring - 1, PIECES)),
            dma((ring - 1, PIECES)),
            dma((peers, PIECES)),
            dma((ring, 2)),
            dma((ring, 4)),
            dma((ring // 2,)),
            dma((ring,)),
            dma((peers,)),
            dma((peers,)),
            dma((peers,)),
            dma((peers,)),
        ],
        compiler_params=pltpu.CompilerParams(has_side_effects=True),
        name="gather_inputs",
    )(tok, wk, wv, add, gates)


def spread_kernel(peers, states, final, bound, f_send, f_recv, b_send, b_recv):
    s, t = lax.axis_index("sp"), lax.axis_index("tp")
    ring = peers // 2
    slot = (s % 2) * ring + s // 2
    x, q = s % 2, s // 2
    y, z = q % 2, q // 2
    deep = ring // 2
    sent = []

    def go(copy):
        copy.start()
        sent.append(copy)

    def pass_on(slot_of, src, to, sem):
        go(remote(src, final.at[slot_of], f_send.at[sem], f_recv.at[slot_of], to, t))

    def arrived(slot_of):
        ref = final.at[slot_of]
        remote(ref, ref, f_send.at[0], f_recv.at[slot_of], s, t).wait_recv()

    own = states.at[peers - 1]
    y_peer, x_peer = 4 * z + 2 * (1 - y) + x, 2 * q + 1 - x
    for off in range(1, deep):
        pass_on(slot, own, 4 * ((z + off) % deep) + 2 * y + x, off)
    pass_on(slot, own, y_peer, deep)
    pass_on(slot, own, x_peer, 2 * deep)
    final[slot] = states[peers - 1]
    for off in range(1, peers):
        to = (s + off) % peers
        go(remote(states.at[to], bound.at[slot], b_send.at[off], b_recv.at[slot], to, t))
    bound[slot] = states[s]
    for off in range(1, deep):
        come = x * ring + 2 * ((z + off) % deep) + y
        arrived(come)
        pass_on(come, final.at[come], y_peer, deep + off)
        pass_on(come, final.at[come], x_peer, 2 * deep + off)
    for off in range(deep):
        come = x * ring + 2 * ((z + off) % deep) + 1 - y
        arrived(come)
        pass_on(come, final.at[come], x_peer, 3 * deep + off)
    for off in range(ring):
        arrived((1 - x) * ring + (q + off) % ring)
    for off in range(1, peers):
        other = (s + off) % peers
        ref = bound.at[(other % 2) * ring + other // 2]
        remote(
            ref, ref, b_send.at[off], b_recv.at[(other % 2) * ring + other // 2], s, t
        ).wait_recv()
    for copy in sent:
        copy.wait_send()


def spread_states(states, peers):
    dma = pltpu.SemaphoreType.DMA
    vmem = pl.BlockSpec(memory_space=pltpu.VMEM)
    return pl.pallas_call(
        lambda *refs: spread_kernel(peers, *refs),
        out_shape=(jax.ShapeDtypeStruct(states.shape, states.dtype),) * 2,
        in_specs=[vmem],
        out_specs=(vmem, vmem),
        scratch_shapes=[dma((peers,))] * 4,
        compiler_params=pltpu.CompilerParams(has_side_effects=True),
        name="spread_states",
    )(states)


def dot32(spec, a, b):
    return jnp.einsum(spec, a, b, precision=lax.Precision.HIGH)


def block_inverse(lower):
    order = lower.shape[-1]
    identity = jnp.eye(order, dtype=jnp.float32)
    result, power = identity - lower, lower
    reached = 2
    while reached < order:
        power = dot32("nij,njk->nik", power, power)
        result = dot32("nij,njk->nik", result, identity + power)
        reached = reached * 2
    return result


def block_states(keys, values, beta, fading):
    blocks, block, width = keys.shape
    cumulative = jnp.cumsum(fading, axis=-1)
    positions = jnp.arange(block)
    strict = positions[:, None] > positions[None, :]
    spread_log = jnp.where(strict, cumulative[:, :, None] - cumulative[:, None, :], 0.0)
    scaled_keys = keys * beta[..., None]
    inner = dot32("nik,njk->nij", scaled_keys, keys)
    inverse = block_inverse(jnp.where(strict, inner * jnp.exp(spread_log), 0.0))
    targets = jnp.concatenate(
        [scaled_keys * jnp.exp(cumulative)[..., None], values * beta[..., None]], axis=-1
    )
    solved = dot32("nij,njk->nik", inverse, targets)
    tail = keys * jnp.exp(cumulative[:, -1:] - cumulative)[..., None]
    maps = dot32("nck,ncj->nkj", tail, solved)
    last = jnp.exp(cumulative[:, -1])[:, None, None]
    moves = last * jnp.eye(width, dtype=jnp.float32) - maps[..., :width]
    pair = jnp.concatenate([moves, maps[..., width:]], axis=-1)
    zero = jnp.zeros((blocks, width, width), jnp.float32)
    reach = 1
    while reach < blocks:
        late = pair[reach:]
        joined = dot32("nij,njk->nik", late[..., :width], pair[:-reach])
        joined = joined + jnp.concatenate([zero[reach:], late[..., width:]], axis=-1)
        pair = jnp.concatenate([pair[:reach], joined], axis=0)
        reach *= 2
    return pair[..., width:]


def per_device_heads(
    layer_source_tokens,
    address_projection,
    content_projection,
    strength_projection,
    fading_driver_projection,
    strength_offset,
    channel_fading_speed,
    added_fading_exponent,
    first_step_probe,
    first_step_address,
    first_step_content,
    first_step_outgate,
    first_step_strength_raw,
    channel_scaling_factor,
    readout_projection,
):
    peers = lax.axis_size("sp")
    head_local = channel_fading_speed.shape[0]
    s, t = lax.axis_index("sp"), lax.axis_index("tp")
    mine = s // 2
    _, length, model_width = layer_source_tokens.shape
    half = model_width // 2
    width = ADDRESS_WIDTH
    gates = jnp.concatenate([strength_projection, fading_driver_projection], axis=1)
    gates = lax.dynamic_slice_in_dim(gates, t * half, half, 0)
    gate_count = gates.shape[1]
    gates = jnp.pad(gates, ((0, 0), (0, -gate_count % 128)))
    projected, added = gather_inputs(
        layer_source_tokens,
        address_projection,
        content_projection,
        jnp.swapaxes(added_fading_exponent, 1, 2),
        gates,
        peers,
    )
    projected = projected.astype(jnp.float32)
    wide = projected[..., : 2 * width]
    gate_sum = projected[..., 2 * width :].reshape(peers * length, -1)
    acted = jax.nn.silu(wide)
    keys = acted[..., :width]
    keys = keys * lax.rsqrt(jnp.sum(keys * keys, axis=-1, keepdims=True) + EPSILON)
    values = acted[..., width:]
    head = t * head_local + mine
    total_heads = strength_projection.shape[1]
    beta_logit = lax.dynamic_slice_in_dim(gate_sum, head, 1, 1).reshape(peers, length)
    alpha_logit = lax.dynamic_slice_in_dim(gate_sum, total_heads + head, 1, 1).reshape(
        peers, length
    )
    beta = jax.nn.sigmoid(beta_logit + lax.dynamic_index_in_dim(strength_offset, mine, 0))
    added_own = lax.dynamic_index_in_dim(added, mine, 1, keepdims=False)
    speed = lax.dynamic_index_in_dim(channel_fading_speed, mine, 0)
    fading = added_own - speed * jax.nn.softplus(alpha_logit)
    states = block_states(keys, values, beta, fading).astype(jnp.bfloat16)
    final, bound = spread_states(states, peers)
    state_cache = final.reshape(2, head_local, width, width)
    boundary_cache = bound.reshape(2, 1, head_local, width, width)
    heads_read = read_heads(
        state_cache,
        first_step_probe,
        first_step_address,
        first_step_content,
        first_step_outgate,
        first_step_strength_raw,
        channel_scaling_factor,
    )
    group_terms = jnp.dot(
        heads_read, readout_projection, preferred_element_type=jnp.float32
    ).astype(jnp.bfloat16)
    return (state_cache, lax.psum(group_terms, "tp"), boundary_cache)


def by_heads(mesh):
    def choose(*args):
        seq_count, length, model_width = args[0].shape
        peers, heads = lax.axis_size("sp"), args[6].shape[0]
        fits = (
            lax.axis_size("tp") == 2
            and seq_count == 2
            and peers == 2 * heads
            and heads % 2 == 0
            and length == BLOCK
            and args[1].shape[0] * peers == model_width
        )
        return per_device_heads(*args) if fits else per_device(*args)

    return choose


def solution(mesh):
    return jax.shard_map(
        by_heads(mesh),
        mesh=mesh,
        in_specs=(
            P(None, "sp", None),
            P("sp", "tp"),
            P("sp", "tp"),
            P(),
            P(),
            P("tp"),
            P("tp"),
            P(None, "sp", "tp"),
            P(None, "tp"),
            P(None, "tp"),
            P(None, "tp"),
            P(None, "tp"),
            P(None, "tp"),
            P(),
            P("tp", "sp"),
        ),
        out_specs=(P(None, "tp", None, None), P(None, "sp"), P(None, "sp", "tp", None, None)),
        check_vma=False,
    )
```
